512 devices in a mesh: grp: 2 (over y), ra: 32 (over z), cb: 8 (over x, core).
Axes of the slice: x: 4, y: 2, z: 32, core: 2. Of those that a mesh axis runs over, the one named last changes fastest.
The devices are a block of a 4x8x32 slice.
Arguments:
- stream: bfloat16 [256, 4096], P('grp', 'ra'), parts along dimension 0, may hold values from -180 to 180
- w_gate: float32 [2, 4096, 11264], P(None, 'ra', 'cb'), may hold values from -0.09375 to 0.09375
- w_up: float32 [2, 4096, 11264], P(None, 'ra', 'cb'), may hold values from -0.09375 to 0.09375
- w_down: float32 [2, 11264, 4096], P(None, 'cb', 'ra'), may hold values from -0.0546875 to 0.0546875
- gate_scale: float32 [2, 11264], P(None, 'cb'), may hold values from 0.5 to 2
- up_scale: float32 [2, 11264], P(None, 'cb'), may hold values from 0.5 to 2
- down_scale: float32 [2, 4096], P(None, 'ra'), may hold values from 0.5 to 2
- pre_gain: float32 [2, 4096], P(None, 'ra'), may hold values from 0.1 to 1.9
- out_gain: float32 [4096], P('ra'), may hold values from 0.1 to 1.9
Outputs:
- normed: bfloat16 [256, 4096], P('grp', 'ra'), parts along dimension 0
The draws below stay inside these ranges and needn't reach their ends.
There are 2 independent parts, one for each index of `grp`. The reference program is written for one: setup_inputs(seed, part) draws one part's arguments, and reference() takes and returns one part's arrays. A program takes and returns all parts, laid end to end along the dimension named above; an argument that names none is the same for every part. Nothing has to cross between parts.
All inputs are finite; a program needn't handle non-finite values.
Results may differ from the reference program's by a relative error of at most 0.018.
Values may be sent and summed in bfloat16 or wider, within the bound.
A program may use at most 64 MiB of HBM per device.

```python
import math
import jax
import jax.numpy as jnp
from jax import lax

D = 4096
FF = 11264
LAYERS = 2
TOK = 128
N_CB = 8


def draw_stream(key, part):
    first = jax.random.fold_in(key, 11)
    second = jax.random.fold_in(key, 12)
    channel = jnp.exp(math.log(3.0) * jnp.arange(D, dtype=jnp.float32) / D)
    base = jnp.clip(jax.random.normal(first, (TOK, D), jnp.float32), -6.0, 6.0)
    rows = jnp.exp(jax.random.uniform(second, (TOK, 1), jnp.float32, 0.0, math.log(10.0)))
    return (base * rows * channel[None, :]).astype(jnp.bfloat16)


def shard_levels(key, extent, split, least, top_value):
    def one(axis_at, blocks):
        heights = jax.random.uniform(jax.random.fold_in(jax.random.fold_in(key, 6), axis_at), (blocks,), jnp.float32, least / len(split), top_value / len(split))
        return jnp.repeat(jnp.exp(heights), extent[axis_at] // blocks).reshape((-1,) + (1,) * (len(extent) - axis_at - 1))

    factor_of = one(*split[0])
    for cut in split[1:]:
        factor_of = factor_of * one(*cut)
    return factor_of


def gaussian(rng, extent, width, most, cuts=(), held_as=jnp.bfloat16):
    level = shard_levels(rng, extent, cuts, -0.22, 0.18) if cuts else 1.0
    array = jax.random.normal(rng, extent, jnp.float32) * width * level
    return jnp.minimum(jnp.maximum(array, -most), most).astype(held_as)


def setup_inputs(seed: int = 0, part: int = 0) -> dict:
    splits = jax.random.split(jax.random.key(seed), 10)
    part_splits = jax.random.split(jax.random.fold_in(splits[9], part), 10)
    stream = draw_stream(jax.random.fold_in(jax.random.fold_in(splits[9], part), 71), part)
    w_gate = gaussian(splits[1], (LAYERS, D, FF), D ** -0.5, 0.09375, ((1, 32), (2, 8)), jnp.float32)
    w_up = gaussian(splits[2], (LAYERS, D, FF), D ** -0.5, 0.09375, ((1, 32), (2, 8)), jnp.float32)
    w_down = gaussian(splits[3], (LAYERS, FF, D), FF ** -0.5, 0.0546875, ((1, 8), (2, 32)), jnp.float32)
    gate_scale = jnp.clip(jnp.exp(math.log(2.0) - 1.3862944 * jax.random.uniform(splits[4], (LAYERS, FF), jnp.float32) ** shard_levels(splits[4], (LAYERS, FF), ((1, 8),), -0.2, 0.2)), 0.5, 2.0)
    up_scale = jnp.clip(jnp.exp(math.log(2.0) - 1.3862944 * jax.random.uniform(splits[5], (LAYERS, FF), jnp.float32) ** shard_levels(splits[5], (LAYERS, FF), ((1, 8),), -0.2, 0.2)), 0.5, 2.0)
    down_scale = jnp.clip(jnp.exp(math.log(2.0) - 1.3862944 * jax.random.uniform(splits[6], (LAYERS, D), jnp.float32) ** shard_levels(splits[6], (LAYERS, D), ((1, 32),), -0.2, 0.2)), 0.5, 2.0)
    pre_gain = jnp.clip(1.0 + 0.18 * jax.random.normal(splits[7], (LAYERS, D), jnp.float32), 0.1, 1.9)
    out_gain = jnp.clip(1.0 + 0.18 * jax.random.normal(splits[8], (D,), jnp.float32), 0.1, 1.9)
    return dict(stream=stream, w_gate=w_gate, w_up=w_up, w_down=w_down, gate_scale=gate_scale, up_scale=up_scale, down_scale=down_scale, pre_gain=pre_gain, out_gain=out_gain)


def reference(stream, w_gate, w_up, w_down, gate_scale, up_scale, down_scale, pre_gain, out_gain):
    current = stream
    for layer in range(LAYERS):
        xvals = lax.optimization_barrier(current).astype(jnp.float32)
        rinv = lax.rsqrt(lax.optimization_barrier(jnp.mean(xvals * xvals, axis=1, keepdims=True)) + 1e-06)
        scaled = (xvals * pre_gain[layer]).astype(jnp.bfloat16)
        gate = jnp.dot(scaled, w_gate[layer].astype(jnp.bfloat16), preferred_element_type=jnp.float32) * rinv * gate_scale[layer]
        upper = jnp.dot(scaled, w_up[layer].astype(jnp.bfloat16), preferred_element_type=jnp.float32) * rinv * up_scale[layer]
        hidden = (jax.nn.silu(gate) * upper).astype(jnp.bfloat16)
        blocks = hidden.astype(jnp.float32).reshape(TOK, N_CB, FF // N_CB)
        down_blocks = w_down[layer].astype(jnp.bfloat16).astype(jnp.float32).reshape(N_CB, FF // N_CB, D)
        partial_value = jnp.einsum('tcf,cfd->ctd', blocks, down_blocks).astype(jnp.bfloat16)
        branch = lax.optimization_barrier(jnp.sum(partial_value.astype(jnp.float32), axis=0)) * down_scale[layer]
        current = (0.5 * xvals + branch).astype(jnp.bfloat16)
    xvals = lax.optimization_barrier(current).astype(jnp.float32)
    rinv = lax.rsqrt(lax.optimization_barrier(jnp.mean(xvals * xvals, axis=1, keepdims=True)) + 1e-06)
    return (xvals * rinv * out_gain).astype(jnp.bfloat16)
```

```python
import functools

import jax
import jax.numpy as jnp
from jax import lax
from jax.experimental import pallas as pl
from jax.experimental.pallas import tpu as pltpu
from jax.sharding import PartitionSpec as P

MESH = pl.DeviceIdType.MESH
F32, BF16 = jnp.float32, jnp.bfloat16
LANES, ROWS = 128, 16

PARENT = {9: 0, -9: 0, 3: 0, -3: 0, 6: 9, 12: 9, 15: 9, -6: -9, -12: -9, -14: -9, -15: -14}
for _c in (0, 3, -3, 6, 9, 12, 15, -6, -9, -12):
    PARENT[_c - 1] = _c
    PARENT[_c + 1] = _c
CHILDREN = {}
for _o, _q in PARENT.items():
    CHILDREN.setdefault(_q, []).append(_o)


def height(o):
    return 0 if o not in CHILDREN else 1 + max(height(c) for c in CHILDREN[o])


def path_length(o):
    return 0 if o == 0 else abs(o - PARENT[o]) + path_length(PARENT[o])


def depth(o):
    return 0 if o == 0 else 1 + depth(PARENT[o])


OFFSETS = sorted(PARENT, key=lambda o: (-depth(o), -path_length(o), o))
EDGE = {o: k for k, o in enumerate(OFFSETS)}
INNER = sorted((o for o in CHILDREN if o != 0), key=lambda o: (height(o), -path_length(o), o))
SLOT = {o: k for k, o in enumerate(INNER)}
DOWN = sorted(PARENT, key=lambda o: (depth(o), -height(o), -path_length(o), o))
PEERS = sorted({s * abs(o - q) for o, q in PARENT.items() for s in (1, -1)})
WINDOWS = ((1, "own"), (-1, "own"), (3, "near"), (-3, "near"), (-6, "near"), (5, "pair"), (-9, "right"), (9, "left"))


def body(n_ra, n_cb, layers, width, eps, refs):
    (x_hbm, wg_hbm, wu_hbm, wd_hbm, gs_hbm, us_hbm, ds_hbm, pg_hbm, og_hbm, o_ref,
     x_in, wg, wu, wd, gs, us, ds, pg, og, wgb, wub, wdb, x_ref, pbuf, rbuf, sbuf, hall, cbuf, ssb, ssr, rcol,
     in_sem, rs_s, rs_r, ag_s, ag_r, cb_s, cb_r, ss_s, ss_r) = refs
    z, me = lax.axis_index("ra"), lax.axis_index("cb")
    ff = wg.shape[2]
    cols = ff // LANES
    tok = x_ref.shape[0]
    ttiles = tok // ROWS
    tiles = cols * ttiles
    take = rbuf.shape[1]

    def at(d):
        return lax.rem(z + (n_ra + d), n_ra)

    def start_of(owner):
        return owner * tiles // n_ra

    barrier = pltpu.get_barrier_semaphore()
    for d in PEERS:
        pl.semaphore_signal(barrier, inc=1, device_id={"ra": at(d)}, device_id_type=MESH)
    for k in range(1, n_cb):
        pl.semaphore_signal(barrier, inc=1, device_id={"cb": lax.rem(me + k, n_cb)}, device_id_type=MESH)

    loads = {}

    def load(name, src, dst):
        loads[name] = pltpu.make_async_copy(src, dst, in_sem.at[len(loads)])
        loads[name].start()

    load("x", x_hbm, x_in)
    load("pg", pg_hbm, pg)
    for l in range(layers):
        load(("wg", l), wg_hbm.at[l], wg.at[l])
        load(("wu", l), wu_hbm.at[l], wu.at[l])
        load(("wd", l), wd_hbm.at[l], wd.at[l])
        if l == 0:
            load("gs", gs_hbm, gs)
            load("us", us_hbm, us)
            load("ds", ds_hbm, ds)
            load("og", og_hbm, og)

    def cast(l, which):
        for name, src, dst in (("wg", wg, wgb), ("wu", wu, wub), ("wd", wd, wdb)):
            if name in which:
                loads[(name, l)].wait()
                dst[l] = src[l].astype(BF16)

    def rs_copy(o, src):
        return pltpu.make_async_remote_copy(
            src_ref=src, dst_ref=rbuf.at[EDGE[o]], send_sem=rs_s.at[EDGE[o]], recv_sem=rs_r.at[EDGE[o]],
            device_id={"ra": at(PARENT[o] - o)}, device_id_type=MESH)

    def ss_copy(k):
        kind = {"own": 0, "near": 1, "pair": 2, "right": 3, "left": 4}[WINDOWS[k][1]]
        return pltpu.make_async_remote_copy(
            src_ref=ssb.at[kind], dst_ref=ssr.at[k], send_sem=ss_s.at[k], recv_sem=ss_r.at[k],
            device_id={"ra": at(WINDOWS[k][0])}, device_id_type=MESH)

    def ss_start(xf):
        own = jnp.sum((xf * xf).T, axis=0, keepdims=True)
        ssb[0] = jnp.broadcast_to(own, ssb.shape[1:])
        for k in (0, 1):
            ss_copy(k).start()

    def ss_near():
        for k in (0, 1):
            ss_copy(k).wait_recv()
        ssb[1] = ssb[0] + ssr[0] + ssr[1]
        ssb[2] = ssb[0] + ssr[0]
        for k in (4, 5, 2, 3):
            ss_copy(k).start()

    def ss_mid():
        for k in (2, 3, 4, 5):
            ss_copy(k).wait_recv()
        nine = ssb[1] + ssr[2] + ssr[3]
        ssb[3] = nine + ssr[4]
        ssb[4] = nine + ssr[5]
        ssb[5] = nine
        for k in (6, 7):
            ss_copy(k).start()

    def ss_end():
        for k in (6, 7):
            ss_copy(k).wait_recv()
        total = ssb[5] + ssr[6] + ssr[7]
        for k in range(len(WINDOWS)):
            ss_copy(k).wait_send()
        rinv = lax.rsqrt(total[0:1] / width + eps)
        return jnp.broadcast_to(rinv, (LANES, tok)).T

    loads["x"].wait()
    x_ref[...] = x_in[...].astype(F32)
    loads["pg"].wait()

    for l in range(layers):
        xf = x_ref[...]
        scaled = (xf * pg[l : l + 1, :]).astype(BF16)
        if l == 0:
            cast(0, ("wg", "wu"))
        for which, w in ((0, wgb), (1, wub)):
            part = jnp.dot(scaled, w[l], preferred_element_type=F32).astype(BF16)
            for j in range(cols):
                pbuf[j * ttiles : (j + 1) * ttiles, which] = part[:, j * LANES : (j + 1) * LANES].reshape(
                    ttiles, ROWS, LANES)
        if l == 0:
            pl.semaphore_wait(barrier, len(PEERS) + n_cb - 1)

        for o in OFFSETS:
            if o not in CHILDREN:
                rs_copy(o, pbuf.at[pl.ds(start_of(at(-o)), take)]).start()
        ss_start(xf)
        if l == 0:
            for name in ("gs", "us", "ds", "og"):
                loads[name].wait()
            cast(0, ("wd",))
            for ll in range(1, layers):
                cast(ll, ("wg", "wu", "wd"))

        def total_of(o):
            acc = pbuf[pl.ds(start_of(at(-o)), take)].astype(F32)
            for c in sorted(CHILDREN[o], key=lambda c: (height(c), c)):
                rs_copy(c, rbuf.at[EDGE[c]]).wait_recv()
                acc = acc + rbuf[EDGE[c]].astype(F32)
            return acc

        level = 0
        for o in INNER:
            if height(o) > level:
                level = height(o)
                if level == 1:
                    ss_near()
                if level == 2:
                    ss_mid()
            sbuf[SLOT[o]] = total_of(o).astype(BF16)
            rs_copy(o, sbuf.at[SLOT[o]]).start()
        rcol[...] = ss_end().reshape(ttiles, ROWS, LANES)
        acc = total_of(0)

        first = start_of(z)
        for k in range(take):
            t = first + k
            i, j = lax.rem(t, ttiles), t // ttiles
            rinv = rcol[i]
            at_j = pl.ds(pl.multiple_of(j * LANES, LANES), LANES)
            gate = acc[k, 0] * rinv * gs[l : l + 1, at_j]
            up = acc[k, 1] * rinv * us[l : l + 1, at_j]
            hall[z, k] = (gate / (1.0 + jnp.exp(-gate)) * up).astype(BF16)

        def ag_copy(o, owner):
            return pltpu.make_async_remote_copy(
                src_ref=hall.at[owner], dst_ref=hall.at[owner], send_sem=ag_s.at[EDGE[o]], recv_sem=ag_r.at[EDGE[o]],
                device_id={"ra": at(o - PARENT[o])}, device_id_type=MESH)

        def pass_on(o):
            for c in DOWN:
                if PARENT[c] == o:
                    ag_copy(c, at(-o)).start()

        pass_on(0)
        for o in OFFSETS:
            rs_copy(o, rbuf.at[EDGE[o]]).wait_send()
        for o in DOWN:
            ag_copy(o, at(-o)).wait_recv()
            if o in CHILDREN:
                pass_on(o)
        place = []
        for t in range(tiles):
            owner = max(p for p in range(n_ra) if start_of(p) <= t)
            place.append((owner, t - start_of(owner)))
        hidden = jnp.concatenate(
            [jnp.concatenate([hall[p, k] for p, k in place[j * ttiles : (j + 1) * ttiles]], axis=0) for j in range(cols)],
            axis=1)
        terms = jnp.dot(hidden, wdb[l], preferred_element_type=F32)
        cbuf[l, me] = terms.astype(BF16)

        def cb_copy(k, slot):
            return pltpu.make_async_remote_copy(
                src_ref=cbuf.at[l, slot], dst_ref=cbuf.at[l, slot], send_sem=cb_s.at[l, k], recv_sem=cb_r.at[l, k],
                device_id={"cb": lax.rem(me + k, n_cb)}, device_id_type=MESH)

        for k in range(1, n_cb):
            cb_copy(k, me).start()
        for o in OFFSETS:
            ag_copy(o, at(-o)).wait_send()
        for k in range(1, n_cb):
            cb_copy(k, lax.rem(me + (n_cb - k), n_cb)).wait_recv()
        branch = cbuf[l, 0].astype(F32)
        for k in range(1, n_cb):
            branch = branch + cbuf[l, k].astype(F32)
        for k in range(1, n_cb):
            cb_copy(k, me).wait_send()
        x_ref[...] = (0.5 * xf + branch * ds[l : l + 1, :]).astype(BF16).astype(F32)

    xf = x_ref[...]
    ss_start(xf)
    ss_near()
    ss_mid()
    o_ref[...] = (xf * ss_end() * og[...]).astype(BF16)


def solution(mesh):
    n_ra, n_cb = mesh.shape["ra"], mesh.shape["cb"]

    def local(stream, w_gate, w_up, w_down, gate_scale, up_scale, down_scale, pre_gain, out_gain):
        layers, d_own, ff = w_gate.shape
        tok = stream.shape[0]
        tiles = (ff // LANES) * (tok // ROWS)
        take = -(-tiles // n_ra)
        edges = len(PARENT)
        dma = pltpu.SemaphoreType.DMA
        scratch = [
            pltpu.VMEM(stream.shape, BF16),
            pltpu.VMEM(w_gate.shape, F32),
            pltpu.VMEM(w_up.shape, F32),
            pltpu.VMEM(w_down.shape, F32),
            pltpu.VMEM(gate_scale.shape, F32),
            pltpu.VMEM(up_scale.shape, F32),
            pltpu.VMEM(down_scale.shape, F32),
            pltpu.VMEM(pre_gain.shape, F32),
            pltpu.VMEM((1, d_own), F32),
            pltpu.VMEM(w_gate.shape, BF16),
            pltpu.VMEM(w_up.shape, BF16),
            pltpu.VMEM(w_down.shape, BF16),
            pltpu.VMEM(stream.shape, F32),
            pltpu.VMEM((tiles, 2, ROWS, LANES), BF16),
            pltpu.VMEM((edges, take, 2, ROWS, LANES), BF16),
            pltpu.VMEM((len(INNER), take, 2, ROWS, LANES), BF16),
            pltpu.VMEM((n_ra, take, ROWS, LANES), BF16),
            pltpu.VMEM((layers, n_cb, tok, d_own), BF16),
            pltpu.VMEM((6, 8, tok), F32),
            pltpu.VMEM((len(WINDOWS), 8, tok), F32),
            pltpu.VMEM((tok // ROWS, ROWS, LANES), F32),
            dma((6 + 3 * layers,)),
            dma((edges,)), dma((edges,)), dma((edges,)), dma((edges,)),
            dma((layers, n_cb)), dma((layers, n_cb)),
            dma((len(WINDOWS),)), dma((len(WINDOWS),)),
        ]
        kernel = functools.partial(body, n_ra, n_cb, layers, n_ra * d_own, 1e-6)
        return pl.pallas_call(
            lambda *refs: kernel(refs),
            out_shape=jax.ShapeDtypeStruct(stream.shape, BF16),
            in_specs=[pl.BlockSpec(memory_space=pl.ANY)] * 9,
            out_specs=pl.BlockSpec(memory_space=pltpu.VMEM),
            scratch_shapes=scratch,
            name="ffn_pair",
            compiler_params=pltpu.CompilerParams(collective_id=0, has_side_effects=True),
        )(stream, w_gate, w_up, w_down, gate_scale, up_scale, down_scale, pre_gain, out_gain.reshape(1, d_own))

    placed = (
        P("grp", "ra"),
        P(None, "ra", "cb"),
        P(None, "ra", "cb"),
        P(None, "cb", "ra"),
        P(None, "cb"),
        P(None, "cb"),
        P(None, "ra"),
        P(None, "ra"),
        P("ra"),
    )
    return jax.shard_map(local, mesh=mesh, in_specs=placed, out_specs=P("grp", "ra"), check_vma=False)
```

```python
import functools

import jax
import jax.numpy as jnp
from jax import lax
from jax.experimental import pallas as pl
from jax.experimental.pallas import tpu as pltpu
from jax.sharding import PartitionSpec as P

MESH = pl.DeviceIdType.MESH
F32, BF16 = jnp.float32, jnp.bfloat16
LANES, ROWS = 128, 16

PARENT = {9: 0, -9: 0, 3: 0, -3: 0, 6: 9, 12: 9, 15: 9, -6: -9, -12: -9, -14: -9, -15: -14}
for _c in (0, 3, -3, 6, 9, 12, 15, -6, -9, -12):
    PARENT[_c - 1] = _c
    PARENT[_c + 1] = _c
CHILDREN = {}
for _o, _q in PARENT.items():
    CHILDREN.setdefault(_q, []).append(_o)


def height(o):
    return 0 if o not in CHILDREN else 1 + max(height(c) for c in CHILDREN[o])


def path_length(o):
    return 0 if o == 0 else abs(o - PARENT[o]) + path_length(PARENT[o])


def depth(o):
    return 0 if o == 0 else 1 + depth(PARENT[o])


OFFSETS = sorted(PARENT, key=lambda o: (-depth(o), -path_length(o), o))
EDGE = {o: k for k, o in enumerate(OFFSETS)}
INNER = sorted((o for o in CHILDREN if o != 0), key=lambda o: (height(o), -path_length(o), o))
SLOT = {o: k for k, o in enumerate(INNER)}
DOWN = sorted(PARENT, key=lambda o: (depth(o), -height(o), -path_length(o), o))
PEERS = sorted({s * abs(o - q) for o, q in PARENT.items() for s in (1, -1)})
WINDOWS = ((1, "own"), (-1, "own"), (3, "near"), (-3, "near"), (-6, "near"), (5, "pair"), (-9, "right"), (9, "left"))


def body(n_ra, n_cb, layers, width, eps, refs):
    (x_hbm, wg_hbm, wu_hbm, wd_hbm, gs_hbm, us_hbm, ds_hbm, pg_hbm, og_hbm, o_ref,
     x_in, wg, wu, wd, gs, us, ds, pg, og, wgb, wub, wdb, x_ref, pbuf, rbuf, sbuf, hall, cbuf, ssb, ssr, rcol,
     in_sem, rs_s, rs_r, ag_s, ag_r, cb_s, cb_r, ss_s, ss_r, fin, fin_s, fin_r) = refs
    z, me = lax.axis_index("ra"), lax.axis_index("cb")
    ff = wg.shape[2]
    cols = ff // LANES
    tok = x_ref.shape[0]
    ttiles = tok // ROWS
    tiles = cols * ttiles
    take = rbuf.shape[1]

    def at(d):
        return lax.rem(z + (n_ra + d), n_ra)

    def start_of(owner):
        return owner * tiles // n_ra

    barrier = pltpu.get_barrier_semaphore()
    for d in PEERS:
        pl.semaphore_signal(barrier, inc=1, device_id={"ra": at(d)}, device_id_type=MESH)
    for k in range(1, n_cb):
        pl.semaphore_signal(barrier, inc=1, device_id={"cb": lax.rem(me + k, n_cb)}, device_id_type=MESH)

    loads = {}

    def load(name, src, dst):
        loads[name] = pltpu.make_async_copy(src, dst, in_sem.at[len(loads)])
        loads[name].start()

    load("x", x_hbm, x_in)
    load("pg", pg_hbm, pg)
    for l in range(layers):
        load(("wg", l), wg_hbm.at[l], wg.at[l])
        load(("wu", l), wu_hbm.at[l], wu.at[l])
        load(("wd", l), wd_hbm.at[l], wd.at[l])
        if l == 0:
            load("gs", gs_hbm, gs)
            load("us", us_hbm, us)
            load("ds", ds_hbm, ds)
            load("og", og_hbm, og)

    def cast(l, which):
        for name, src, dst in (("wg", wg, wgb), ("wu", wu, wub), ("wd", wd, wdb)):
            if name in which:
                loads[(name, l)].wait()
                dst[l] = src[l].astype(BF16)

    def rs_copy(o, src):
        return pltpu.make_async_remote_copy(
            src_ref=src, dst_ref=rbuf.at[EDGE[o]], send_sem=rs_s.at[EDGE[o]], recv_sem=rs_r.at[EDGE[o]],
            device_id={"ra": at(PARENT[o] - o)}, device_id_type=MESH)

    def ss_copy(k):
        kind = {"own": 0, "near": 1, "pair": 2, "right": 3, "left": 4}[WINDOWS[k][1]]
        return pltpu.make_async_remote_copy(
            src_ref=ssb.at[kind], dst_ref=ssr.at[k], send_sem=ss_s.at[k], recv_sem=ss_r.at[k],
            device_id={"ra": at(WINDOWS[k][0])}, device_id_type=MESH)

    def ss_start(xf):
        own = jnp.sum((xf * xf).T, axis=0, keepdims=True)
        ssb[0] = jnp.broadcast_to(own, ssb.shape[1:])
        for k in (0, 1):
            ss_copy(k).start()

    def ss_near():
        for k in (0, 1):
            ss_copy(k).wait_recv()
        ssb[1] = ssb[0] + ssr[0] + ssr[1]
        ssb[2] = ssb[0] + ssr[0]
        for k in (4, 5, 2, 3):
            ss_copy(k).start()

    def ss_mid():
        for k in (2, 3, 4, 5):
            ss_copy(k).wait_recv()
        nine = ssb[1] + ssr[2] + ssr[3]
        ssb[3] = nine + ssr[4]
        ssb[4] = nine + ssr[5]
        ssb[5] = nine
        for k in (6, 7):
            ss_copy(k).start()

    def ss_end():
        for k in (6, 7):
            ss_copy(k).wait_recv()
        total = ssb[5] + ssr[6] + ssr[7]
        for k in range(len(WINDOWS)):
            ss_copy(k).wait_send()
        rinv = lax.rsqrt(total[0:1] / width + eps)
        return jnp.broadcast_to(rinv, (LANES, tok)).T

    loads["x"].wait()
    x_ref[...] = x_in[...].astype(F32)

    for l in range(layers):
        xf = x_ref[...]
        if l == 0:
            pl.semaphore_wait(barrier, len(PEERS) + n_cb - 1)
        ss_start(xf)
        if l == 0:
            loads["pg"].wait()
            cast(0, ("wg", "wu"))
        scaled = (xf * pg[l : l + 1, :]).astype(BF16)
        for which, w in ((0, wgb), (1, wub)):
            part = jnp.dot(scaled, w[l], preferred_element_type=F32).astype(BF16)
            for j in range(cols):
                pbuf[j * ttiles : (j + 1) * ttiles, which] = part[:, j * LANES : (j + 1) * LANES].reshape(
                    ttiles, ROWS, LANES)

        for o in OFFSETS:
            if o not in CHILDREN:
                rs_copy(o, pbuf.at[pl.ds(start_of(at(-o)), take)]).start()
        ss_near()
        if l == 0:
            for name in ("gs", "us", "ds", "og"):
                loads[name].wait()
            cast(0, ("wd",))
            for ll in range(1, layers):
                cast(ll, ("wg", "wu", "wd"))

        def total_of(o):
            acc = pbuf[pl.ds(start_of(at(-o)), take)].astype(F32)
            for c in sorted(CHILDREN[o], key=lambda c: (height(c), c)):
                rs_copy(c, rbuf.at[EDGE[c]]).wait_recv()
                acc = acc + rbuf[EDGE[c]].astype(F32)
            return acc

        level = 0
        for o in INNER:
            if height(o) > level:
                level = height(o)
                if level == 2:
                    ss_mid()
            sbuf[SLOT[o]] = total_of(o).astype(BF16)
            rs_copy(o, sbuf.at[SLOT[o]]).start()
        rcol[...] = ss_end().reshape(ttiles, ROWS, LANES)
        acc = total_of(0)

        first = start_of(z)
        for k in range(take):
            t = first + k
            i, j = lax.rem(t, ttiles), t // ttiles
            rinv = rcol[i]
            at_j = pl.ds(pl.multiple_of(j * LANES, LANES), LANES)
            gate = acc[k, 0] * rinv * gs[l : l + 1, at_j]
            up = acc[k, 1] * rinv * us[l : l + 1, at_j]
            hall[z, k] = (gate / (1.0 + jnp.exp(-gate)) * up).astype(BF16)

        def ag_copy(o, owner):
            return pltpu.make_async_remote_copy(
                src_ref=hall.at[owner], dst_ref=hall.at[owner], send_sem=ag_s.at[EDGE[o]], recv_sem=ag_r.at[EDGE[o]],
                device_id={"ra": at(o - PARENT[o])}, device_id_type=MESH)

        def pass_on(o):
            for c in DOWN:
                if PARENT[c] == o:
                    ag_copy(c, at(-o)).start()

        pass_on(0)
        for o in OFFSETS:
            rs_copy(o, rbuf.at[EDGE[o]]).wait_send()
        for o in DOWN:
            ag_copy(o, at(-o)).wait_recv()
            if o in CHILDREN:
                pass_on(o)
        place = []
        for t in range(tiles):
            owner = max(p for p in range(n_ra) if start_of(p) <= t)
            place.append((owner, t - start_of(owner)))
        hidden = jnp.concatenate(
            [jnp.concatenate([hall[p, k] for p, k in place[j * ttiles : (j + 1) * ttiles]], axis=0) for j in range(cols)],
            axis=1)
        terms = jnp.dot(hidden, wdb[l], preferred_element_type=F32)
        cbuf[l, me] = terms.astype(BF16)

        def cb_copy(k, slot):
            return pltpu.make_async_remote_copy(
                src_ref=cbuf.at[l, slot], dst_ref=cbuf.at[l, slot], send_sem=cb_s.at[l, k], recv_sem=cb_r.at[l, k],
                device_id={"cb": lax.rem(me + k, n_cb)}, device_id_type=MESH)

        for k in range(1, n_cb):
            cb_copy(k, me).start()
        for o in OFFSETS:
            ag_copy(o, at(-o)).wait_send()
        for k in range(1, n_cb):
            cb_copy(k, lax.rem(me + (n_cb - k), n_cb)).wait_recv()
        branch = cbuf[l, 0].astype(F32)
        for k in range(1, n_cb):
            branch = branch + cbuf[l, k].astype(F32)
        for k in range(1, n_cb):
            cb_copy(k, me).wait_send()
        x_ref[...] = (0.5 * xf + branch * ds[l : l + 1, :]).astype(BF16).astype(F32)

    xf = x_ref[...]
    fin[0:1] = jnp.sum((xf * xf).T, axis=0, keepdims=True)

    def fin_copy(d):
        k = d % n_ra
        return pltpu.make_async_remote_copy(
            src_ref=fin.at[pl.ds(0, 1)], dst_ref=fin.at[pl.ds(k, 1)], send_sem=fin_s.at[k], recv_sem=fin_r.at[k],
            device_id={"ra": at(d)}, device_id_type=MESH)

    far = [s * d for d in range(n_ra // 2, 0, -1) for s in (1, -1) if 2 * d < n_ra or s > 0]
    for d in far:
        fin_copy(d).start()
    scaled = xf * og[...]
    for d in far:
        fin_copy(d).wait_recv()
    rinv = lax.rsqrt(jnp.sum(fin[...], axis=0, keepdims=True) / width + eps)
    o_ref[...] = (scaled * jnp.broadcast_to(rinv, (LANES, tok)).T).astype(BF16)
    for d in far:
        fin_copy(d).wait_send()


def solution(mesh):
    n_ra, n_cb = mesh.shape["ra"], mesh.shape["cb"]

    def local(stream, w_gate, w_up, w_down, gate_scale, up_scale, down_scale, pre_gain, out_gain):
        layers, d_own, ff = w_gate.shape
        tok = stream.shape[0]
        tiles = (ff // LANES) * (tok // ROWS)
        take = -(-tiles // n_ra)
        edges = len(PARENT)
        dma = pltpu.SemaphoreType.DMA
        scratch = [
            pltpu.VMEM(stream.shape, BF16),
            pltpu.VMEM(w_gate.shape, F32),
            pltpu.VMEM(w_up.shape, F32),
            pltpu.VMEM(w_down.shape, F32),
            pltpu.VMEM(gate_scale.shape, F32),
            pltpu.VMEM(up_scale.shape, F32),
            pltpu.VMEM(down_scale.shape, F32),
            pltpu.VMEM(pre_gain.shape, F32),
            pltpu.VMEM((1, d_own), F32),
            pltpu.VMEM(w_gate.shape, BF16),
            pltpu.VMEM(w_up.shape, BF16),
            pltpu.VMEM(w_down.shape, BF16),
            pltpu.VMEM(stream.shape, F32),
            pltpu.VMEM((tiles, 2, ROWS, LANES), BF16),
            pltpu.VMEM((edges, take, 2, ROWS, LANES), BF16),
            pltpu.VMEM((len(INNER), take, 2, ROWS, LANES), BF16),
            pltpu.VMEM((n_ra, take, ROWS, LANES), BF16),
            pltpu.VMEM((layers, n_cb, tok, d_own), BF16),
            pltpu.VMEM((6, 8, tok), F32),
            pltpu.VMEM((len(WINDOWS), 8, tok), F32),
            pltpu.VMEM((tok // ROWS, ROWS, LANES), F32),
            dma((6 + 3 * layers,)),
            dma((edges,)), dma((edges,)), dma((edges,)), dma((edges,)),
            dma((layers, n_cb)), dma((layers, n_cb)),
            dma((len(WINDOWS),)), dma((len(WINDOWS),)),
            pltpu.VMEM((n_ra, tok), F32), dma((n_ra,)), dma((n_ra,)),
        ]
        kernel = functools.partial(body, n_ra, n_cb, layers, n_ra * d_own, 1e-6)
        return pl.pallas_call(
            lambda *refs: kernel(refs),
            out_shape=jax.ShapeDtypeStruct(stream.shape, BF16),
            in_specs=[pl.BlockSpec(memory_space=pl.ANY)] * 9,
            out_specs=pl.BlockSpec(memory_space=pltpu.VMEM),
            scratch_shapes=scratch,
            name="ffn_pair",
            compiler_params=pltpu.CompilerParams(collective_id=0, has_side_effects=True),
        )(stream, w_gate, w_up, w_down, gate_scale, up_scale, down_scale, pre_gain, out_gain.reshape(1, d_own))

    placed = (
        P("grp", "ra"),
        P(None, "ra", "cb"),
        P(None, "ra", "cb"),
        P(None, "cb", "ra"),
        P(None, "cb"),
        P(None, "cb"),
        P(None, "ra"),
        P(None, "ra"),
        P("ra"),
    )
    return jax.shard_map(local, mesh=mesh, in_specs=placed, out_specs=P("grp", "ra"), check_vma=False)
```

```python
import functools

import jax
import jax.numpy as jnp
from jax import lax
from jax.experimental import pallas as pl
from jax.experimental.pallas import tpu as pltpu
from jax.sharding import PartitionSpec as P

MESH = pl.DeviceIdType.MESH
F32, BF16 = jnp.float32, jnp.bfloat16
LANES, ROWS = 128, 16

UP = {14: 15, 16: 15, -15: -14, -13: -12, -11: -12, -7: -6, -5: -6, 5: 6, 7: 6, 11: 12, 13: 12, -10: -9, -8: -9, 8:
    9, 10: 9, -4: -3, -2: -3, 2: 3, 4: 3, -1: 0, 1: 0, 15: 9, -14: -9, -12: -9, -6: -9, 6: 9, 12: 9, -3: 0, 3: 0,
    -9: 0, 9: 0}
DOWN = {-9: 0, 9: 0, -3: 0, 3: 0, -1: 0, 1: 0, 15: 9, -14: -9, -12: -9, -6: -9, 6: 9, 12: 9, -10: -9, -8: -9, 8: 9,
    10: 9, -4: -3, -2: -3, 2: 3, 4: 3, 14: 15, 16: 15, -15: -14, -13: -12, -11: -12, -7: -6, -5: -6, 5: 6, 7: 6,
    11: 12, 13: 12}
SUMMED = {}
for _o, _q in UP.items():
    SUMMED.setdefault(_q, []).append(_o)
EDGE = {o: k for k, o in enumerate(c for q in SUMMED for c in SUMMED[q])}
NODE = {q: k for k, q in enumerate(SUMMED)}
LEAVES = [o for o in UP if o not in SUMMED]
INNER = [o for o in UP if o in SUMMED]


def height(o):
    return 0 if o not in SUMMED else 1 + max(height(c) for c in SUMMED[o])


WINDOWS = ((1, "own"), (-1, "own"), (3, "near"), (-3, "near"), (-6, "near"), (5, "pair"), (-9, "right"), (9, "left"))
REACH = {abs(o - q) for tree in (UP, DOWN) for o, q in tree.items()} | {abs(d) for d, _ in WINDOWS}
PEERS = sorted(s * d for d in REACH for s in (1, -1))


def body(n_ra, n_cb, layers, width, eps, refs):
    (x_hbm, wg_hbm, wu_hbm, wd_hbm, gs_hbm, us_hbm, ds_hbm, pg_hbm, og_hbm, o_ref,
     x_in, wg, wu, wd, gs, us, ds, pg, og, wgb, wub, wdb, x_ref, pbuf, rbuf, sbuf, hall, cbuf, ssb, ssr, rcol,
     in_sem, rs_s, rs_r, ag_s, ag_r, cb_s, cb_r, ss_s, ss_r, fin, fin_s, fin_r) = refs
    z, me = lax.axis_index("ra"), lax.axis_index("cb")
    ff = wg.shape[2]
    cols = ff // LANES
    tok = x_ref.shape[0]
    ttiles = tok // ROWS
    tiles = cols * ttiles
    take = rbuf.shape[1]

    def at(d):
        return lax.rem(z + (n_ra + d), n_ra)

    def start_of(owner):
        return owner * tiles // n_ra

    barrier = pltpu.get_barrier_semaphore()
    for d in PEERS:
        pl.semaphore_signal(barrier, inc=1, device_id={"ra": at(d)}, device_id_type=MESH)
    for k in range(1, n_cb):
        pl.semaphore_signal(barrier, inc=1, device_id={"cb": lax.rem(me + k, n_cb)}, device_id_type=MESH)

    loads = {}

    def load(name, src, dst):
        loads[name] = pltpu.make_async_copy(src, dst, in_sem.at[len(loads)])
        loads[name].start()

    load("x", x_hbm, x_in)
    load("pg", pg_hbm, pg)
    for l in range(layers):
        load(("wg", l), wg_hbm.at[l], wg.at[l])
        load(("wu", l), wu_hbm.at[l], wu.at[l])
        load(("wd", l), wd_hbm.at[l], wd.at[l])
        if l == 0:
            load("gs", gs_hbm, gs)
            load("us", us_hbm, us)
            load("ds", ds_hbm, ds)
            load("og", og_hbm, og)

    def wait_for(ref, sem):
        pltpu.make_async_copy(ref, ref, sem).wait()

    def cast(l, which):
        for name, src, dst in (("wg", wg, wgb), ("wu", wu, wub), ("wd", wd, wdb)):
            if name in which:
                loads[(name, l)].wait()
                dst[l] = src[l].astype(BF16)

    def rs_copy(o, src):
        return pltpu.make_async_remote_copy(
            src_ref=src, dst_ref=rbuf.at[EDGE[o]], send_sem=rs_s, recv_sem=rs_r.at[NODE[UP[o]]],
            device_id={"ra": at(UP[o] - o)}, device_id_type=MESH)

    def ss_copy(k):
        kind = {"own": 0, "near": 1, "pair": 2, "right": 3, "left": 4}[WINDOWS[k][1]]
        return pltpu.make_async_remote_copy(
            src_ref=ssb.at[kind], dst_ref=ssr.at[k], send_sem=ss_s, recv_sem=ss_r.at[k],
            device_id={"ra": at(WINDOWS[k][0])}, device_id_type=MESH)

    def ss_own(xf):
        own = jnp.sum((xf * xf).T, axis=0, keepdims=True)
        ssb[0] = jnp.broadcast_to(own, ssb.shape[1:])

    def ss_start():
        for k in (0, 1):
            ss_copy(k).start()

    def ss_near():
        for k in (0, 1):
            ss_copy(k).wait_recv()
        ssb[1] = ssb[0] + ssr[0] + ssr[1]
        ssb[2] = ssb[0] + ssr[0]
        for k in (4, 5, 2, 3):
            ss_copy(k).start()

    def ss_mid():
        for k in (2, 3, 4, 5):
            ss_copy(k).wait_recv()
        nine = ssb[1] + ssr[2] + ssr[3]
        ssb[3] = nine + ssr[4]
        ssb[4] = nine + ssr[5]
        ssb[5] = nine
        for k in (6, 7):
            ss_copy(k).start()

    def ss_end():
        for k in (6, 7):
            ss_copy(k).wait_recv()
        total = ssb[5] + ssr[6] + ssr[7]
        rinv = lax.rsqrt(total[0:1] / width + eps)
        return jnp.broadcast_to(rinv, (LANES, tok)).T

    loads["x"].wait()
    x_ref[...] = x_in[...].astype(F32)

    for l in range(layers):
        xf = x_ref[...]
        ss_own(xf)
        if l > 0:
            ss_start()
        if l == 0:
            loads["pg"].wait()
            cast(0, ("wg", "wu"))
        scaled = (xf * pg[l : l + 1, :]).astype(BF16)
        for which, w in ((0, wgb), (1, wub)):
            part = jnp.dot(scaled, w[l], preferred_element_type=F32).astype(BF16)
            for j in range(cols):
                pbuf[j * ttiles : (j + 1) * ttiles, which] = part[:, j * LANES : (j + 1) * LANES].reshape(
                    ttiles, ROWS, LANES)
        if l == 0:
            pl.semaphore_wait(barrier, len(PEERS) + n_cb - 1)
            ss_start()

        for o in LEAVES:
            rs_copy(o, pbuf.at[pl.ds(start_of(at(-o)), take)]).start()
        if l == 0:
            for name in ("gs", "us", "ds", "og"):
                loads[name].wait()
            cast(0, ("wd",))
            for ll in range(1, layers):
                cast(ll, ("wg", "wu", "wd"))
        ss_near()

        def total_of(o):
            wait_for(rbuf.at[pl.ds(EDGE[SUMMED[o][0]], len(SUMMED[o]))], rs_r.at[NODE[o]])
            acc = pbuf[pl.ds(start_of(at(-o)), take)].astype(F32)
            for c in SUMMED[o]:
                acc = acc + rbuf[EDGE[c]].astype(F32)
            return acc

        nears = sum(height(o) == 1 for o in INNER)
        slot = {o: k for k, o in enumerate(INNER)}
        for n, o in enumerate(INNER):
            if n == nears:
                ss_mid()
            sbuf[slot[o]] = total_of(o).astype(BF16)
            rs_copy(o, sbuf.at[slot[o]]).start()
        rcol[...] = ss_end().reshape(ttiles, ROWS, LANES)
        acc = total_of(0)

        first = start_of(z)
        for k in range(take):
            t = first + k
            i, j = lax.rem(t, ttiles), t // ttiles
            rinv = rcol[i]
            at_j = pl.ds(pl.multiple_of(j * LANES, LANES), LANES)
            gate = acc[k, 0] * rinv * gs[l : l + 1, at_j]
            up = acc[k, 1] * rinv * us[l : l + 1, at_j]
            hall[z, k] = (gate / (1.0 + jnp.exp(-gate)) * up).astype(BF16)

        forwards = set(DOWN.values())

        def ag_copy(o, owner):
            return pltpu.make_async_remote_copy(
                src_ref=hall.at[owner], dst_ref=hall.at[owner], send_sem=ag_s, recv_sem=ag_r.at[EDGE[o] if o in forwards else len(EDGE)],
                device_id={"ra": at(o - DOWN[o])}, device_id_type=MESH)

        def pass_on(o):
            for c in DOWN:
                if DOWN[c] == o:
                    ag_copy(c, at(-o)).start()

        pass_on(0)
        for o in DOWN:
            if o in forwards:
                ag_copy(o, at(-o)).wait_recv()
                pass_on(o)
        wait_for(hall.at[pl.ds(0, sum(o not in forwards for o in DOWN))], ag_r.at[len(EDGE)])
        place = []
        for t in range(tiles):
            owner = max(p for p in range(n_ra) if start_of(p) <= t)
            place.append((owner, t - start_of(owner)))
        hidden = jnp.concatenate(
            [jnp.concatenate([hall[p, k] for p, k in place[j * ttiles : (j + 1) * ttiles]], axis=0) for j in range(cols)],
            axis=1)
        terms = jnp.dot(hidden, wdb[l], preferred_element_type=F32)
        cbuf[l, me] = terms.astype(BF16)

        def cb_copy(k, slot):
            return pltpu.make_async_remote_copy(
                src_ref=cbuf.at[l, slot], dst_ref=cbuf.at[l, slot], send_sem=cb_s.at[l], recv_sem=cb_r.at[l],
                device_id={"cb": lax.rem(me + k, n_cb)}, device_id_type=MESH)

        for k in range(1, n_cb):
            cb_copy(k, me).start()
        wait_for(rbuf, rs_s)
        wait_for(ssr, ss_s)
        wait_for(hall.at[pl.ds(0, len(DOWN))], ag_s)
        wait_for(cbuf.at[l, pl.ds(0, n_cb - 1)], cb_r.at[l])
        branch = cbuf[l, 0].astype(F32)
        for k in range(1, n_cb):
            branch = branch + cbuf[l, k].astype(F32)
        wait_for(cbuf.at[l, pl.ds(0, n_cb - 1)], cb_s.at[l])
        x_ref[...] = (0.5 * xf + branch * ds[l : l + 1, :]).astype(BF16).astype(F32)

    xf = x_ref[...]
    fin[0:1] = jnp.sum((xf * xf).T, axis=0, keepdims=True)

    def fin_copy(d):
        k = d % n_ra
        return pltpu.make_async_remote_copy(
            src_ref=fin.at[pl.ds(0, 1)], dst_ref=fin.at[pl.ds(k, 1)], send_sem=fin_s, recv_sem=fin_r,
            device_id={"ra": at(d)}, device_id_type=MESH)

    far = [s * d for d in range(n_ra // 2, 0, -1) for s in (1, -1) if 2 * d < n_ra or s > 0]
    for d in far:
        fin_copy(d).start()
    scaled = xf * og[...]
    wait_for(fin.at[pl.ds(0, n_ra - 1)], fin_r)
    rinv = lax.rsqrt(jnp.sum(fin[...], axis=0, keepdims=True) / width + eps)
    o_ref[...] = (scaled * jnp.broadcast_to(rinv, (LANES, tok)).T).astype(BF16)
    wait_for(fin.at[pl.ds(0, n_ra - 1)], fin_s)


def solution(mesh):
    n_ra, n_cb = mesh.shape["ra"], mesh.shape["cb"]

    def local(stream, w_gate, w_up, w_down, gate_scale, up_scale, down_scale, pre_gain, out_gain):
        layers, d_own, ff = w_gate.shape
        tok = stream.shape[0]
        tiles = (ff // LANES) * (tok // ROWS)
        take = -(-tiles // n_ra)
        edges = len(EDGE)
        dma = pltpu.SemaphoreType.DMA
        scratch = [
            pltpu.VMEM(stream.shape, BF16),
            pltpu.VMEM(w_gate.shape, F32),
            pltpu.VMEM(w_up.shape, F32),
            pltpu.VMEM(w_down.shape, F32),
            pltpu.VMEM(gate_scale.shape, F32),
            pltpu.VMEM(up_scale.shape, F32),
            pltpu.VMEM(down_scale.shape, F32),
            pltpu.VMEM(pre_gain.shape, F32),
            pltpu.VMEM((1, d_own), F32),
            pltpu.VMEM(w_gate.shape, BF16),
            pltpu.VMEM(w_up.shape, BF16),
            pltpu.VMEM(w_down.shape, BF16),
            pltpu.VMEM(stream.shape, F32),
            pltpu.VMEM((tiles, 2, ROWS, LANES), BF16),
            pltpu.VMEM((edges, take, 2, ROWS, LANES), BF16),
            pltpu.VMEM((len(INNER), take, 2, ROWS, LANES), BF16),
            pltpu.VMEM((n_ra, take, ROWS, LANES), BF16),
            pltpu.VMEM((layers, n_cb, tok, d_own), BF16),
            pltpu.VMEM((6, 8, tok), F32),
            pltpu.VMEM((len(WINDOWS), 8, tok), F32),
            pltpu.VMEM((tok // ROWS, ROWS, LANES), F32),
            dma((6 + 3 * layers,)),
            dma, dma((len(NODE),)), dma, dma((edges + 1,)),
            dma((layers,)), dma((layers,)),
            dma, dma((len(WINDOWS),)),
            pltpu.VMEM((n_ra, tok), F32), dma, dma,
        ]
        kernel = functools.partial(body, n_ra, n_cb, layers, n_ra * d_own, 1e-6)
        return pl.pallas_call(
            lambda *refs: kernel(refs),
            out_shape=jax.ShapeDtypeStruct(stream.shape, BF16),
            in_specs=[pl.BlockSpec(memory_space=pl.ANY)] * 9,
            out_specs=pl.BlockSpec(memory_space=pltpu.VMEM),
            scratch_shapes=scratch,
            name="ffn_pair",
            compiler_params=pltpu.CompilerParams(collective_id=0, has_side_effects=True),
        )(stream, w_gate, w_up, w_down, gate_scale, up_scale, down_scale, pre_gain, out_gain.reshape(1, d_own))

    placed = (
        P("grp", "ra"),
        P(None, "ra", "cb"),
        P(None, "ra", "cb"),
        P(None, "cb", "ra"),
        P(None, "cb"),
        P(None, "cb"),
        P(None, "ra"),
        P(None, "ra"),
        P("ra"),
    )
    return jax.shard_map(local, mesh=mesh, in_specs=placed, out_specs=P("grp", "ra"), check_vma=False)
```

```python
import functools

import jax
import jax.numpy as jnp
from jax import lax
from jax.experimental import pallas as pl
from jax.experimental.pallas import tpu as pltpu
from jax.sharding import PartitionSpec as P

MESH = pl.DeviceIdType.MESH
F32, BF16 = jnp.float32, jnp.bfloat16
LANES, ROWS = 128, 16

UP = {15: 16, -7: -6, -13: -14, -4: -5, 12: 13, -12: -9, 5: 4, -15: -14, 2: 1, 11: 10, 14: 13, 7: 8, -11: -10,
    16: 13, 3: 4, 1: 0, -8: -9, -6: -5, 6: 4, -14: -9, -1: -2, 13: 9, -10: -9, 8: 9, -5: -3, 10: 9, 4: 0, -9: 0,
    -2: -3, 9: 0, -3: 0}
DOWN = {9: 0, -4: 0, -9: 0, 7: 0, -11: -4, -7: -4, -2: -4, 2: 0, -3: -4, 3: 0, 6: 7, 1: 0, 8: 7, 12: 9, -12: -9, 10: 9,
    16: 9, -15: -9, -6: -7, 4: 6, 5: 6, -10: -9, -8: -7, -1: 0, 13: 9, 15: 12, 14: 12, 11: 10, -5: -4, -13: -12,
    -14: -12}
SUMMED = {}
for _o, _q in UP.items():
    SUMMED.setdefault(_q, []).append(_o)
EDGE = {o: k for k, o in enumerate(c for q in SUMMED for c in SUMMED[q])}
NODE = {q: k for k, q in enumerate(SUMMED)}
INNER = [o for o in UP if o in SUMMED]
WINDOWS = ((1, "own"), (-1, "own"), (3, "near"), (-3, "near"), (-6, "near"), (5, "pair"), (-9, "right"), (9, "left"))
REACH = {abs(o - q) for tree in (UP, DOWN) for o, q in tree.items()} | {abs(d) for d, _ in WINDOWS}
PEERS = sorted(s * d for d in REACH for s in (1, -1))


def body(n_ra, n_cb, layers, width, eps, refs):
    (x_hbm, wg_hbm, wu_hbm, wd_hbm, gs_hbm, us_hbm, ds_hbm, pg_hbm, og_hbm, o_ref,
     x_in, wg, wu, wd, gs, us, ds, pg, og, wgb, wub, wdb, x_ref, pbuf, rbuf, sbuf, hall, cbuf, ssb, ssr, rcol,
     in_sem, rs_s, rs_r, ag_s, ag_r, cb_s, cb_r, ss_s, ss_r, fin, fin_s, fin_r) = refs
    z, me = lax.axis_index("ra"), lax.axis_index("cb")
    ff = wg.shape[2]
    cols = ff // LANES
    tok = x_ref.shape[0]
    ttiles = tok // ROWS
    tiles = cols * ttiles
    take = rbuf.shape[1]

    def at(d):
        return lax.rem(z + (n_ra + d), n_ra)

    def start_of(owner):
        return owner * tiles // n_ra

    barrier = pltpu.get_barrier_semaphore()
    for d in PEERS:
        pl.semaphore_signal(barrier, inc=1, device_id={"ra": at(d)}, device_id_type=MESH)
    for k in range(1, n_cb):
        pl.semaphore_signal(barrier, inc=1, device_id={"cb": lax.rem(me + k, n_cb)}, device_id_type=MESH)

    loads = {}

    def load(name, src, dst):
        loads[name] = pltpu.make_async_copy(src, dst, in_sem.at[len(loads)])
        loads[name].start()

    load("x", x_hbm, x_in)
    load("pg", pg_hbm, pg)
    load(("wg", 0), wg_hbm.at[0], wg.at[0])
    load(("wu", 0), wu_hbm.at[0], wu.at[0])

    def load_rest():
        load("gs", gs_hbm, gs)
        load("us", us_hbm, us)
        load("ds", ds_hbm, ds)
        load("og", og_hbm, og)
        load(("wd", 0), wd_hbm.at[0], wd.at[0])
        for l in range(1, layers):
            load(("wg", l), wg_hbm.at[l], wg.at[l])
            load(("wu", l), wu_hbm.at[l], wu.at[l])
            load(("wd", l), wd_hbm.at[l], wd.at[l])

    def wait_for(ref, sem):
        pltpu.make_async_copy(ref, ref, sem).wait()

    def cast(l, which):
        for name, src, dst in (("wg", wg, wgb), ("wu", wu, wub), ("wd", wd, wdb)):
            if name in which:
                loads[(name, l)].wait()
                dst[l] = src[l].astype(BF16)

    def rs_copy(o, src):
        return pltpu.make_async_remote_copy(
            src_ref=src, dst_ref=rbuf.at[EDGE[o]], send_sem=rs_s, recv_sem=rs_r.at[NODE[UP[o]]],
            device_id={"ra": at(UP[o] - o)}, device_id_type=MESH)

    def ss_copy(k):
        kind = {"own": 0, "near": 1, "pair": 2, "right": 3, "left": 4}[WINDOWS[k][1]]
        return pltpu.make_async_remote_copy(
            src_ref=ssb.at[kind], dst_ref=ssr.at[k], send_sem=ss_s, recv_sem=ss_r.at[k],
            device_id={"ra": at(WINDOWS[k][0])}, device_id_type=MESH)

    def ss_own(xf):
        own = jnp.sum((xf * xf).T, axis=0, keepdims=True)
        ssb[0] = jnp.broadcast_to(own, ssb.shape[1:])

    def ss_start():
        for k in (0, 1):
            ss_copy(k).start()

    def ss_near():
        for k in (0, 1):
            ss_copy(k).wait_recv()
        ssb[1] = ssb[0] + ssr[0] + ssr[1]
        ssb[2] = ssb[0] + ssr[0]
        for k in (4, 5, 2, 3):
            ss_copy(k).start()

    def ss_mid():
        for k in (2, 3, 4, 5):
            ss_copy(k).wait_recv()
        nine = ssb[1] + ssr[2] + ssr[3]
        ssb[3] = nine + ssr[4]
        ssb[4] = nine + ssr[5]
        ssb[5] = nine
        for k in (6, 7):
            ss_copy(k).start()

    def ss_end():
        for k in (6, 7):
            ss_copy(k).wait_recv()
        total = ssb[5] + ssr[6] + ssr[7]
        rinv = lax.rsqrt(total[0:1] / width + eps)
        return jnp.broadcast_to(rinv, (LANES, tok)).T

    loads["x"].wait()
    x_ref[...] = x_in[...].astype(F32)

    for l in range(layers):
        xf = x_ref[...]
        ss_own(xf)
        if l > 0:
            ss_start()
        if l == 0:
            loads["pg"].wait()
            cast(0, ("wg", "wu"))
        scaled = (xf * pg[l : l + 1, :]).astype(BF16)
        for which, w in ((0, wgb), (1, wub)):
            part = jnp.dot(scaled, w[l], preferred_element_type=F32).astype(BF16)
            for j in range(cols):
                pbuf[j * ttiles : (j + 1) * ttiles, which] = part[:, j * LANES : (j + 1) * LANES].reshape(
                    ttiles, ROWS, LANES)
        if l == 0:
            pl.semaphore_wait(barrier, len(PEERS) + n_cb - 1)
            ss_start()

        def total_of(o):
            wait_for(rbuf.at[pl.ds(EDGE[SUMMED[o][0]], len(SUMMED[o]))], rs_r.at[NODE[o]])
            acc = pbuf[pl.ds(start_of(at(-o)), take)].astype(F32)
            for c in SUMMED[o]:
                acc = acc + rbuf[EDGE[c]].astype(F32)
            return acc

        for o in UP:
            if o not in SUMMED:
                rs_copy(o, pbuf.at[pl.ds(start_of(at(-o)), take)]).start()
                continue
            n = INNER.index(o)
            if n == 0:
                if l == 0:
                    load_rest()
                ss_near()
            if n == len(INNER) // 2:
                ss_mid()
            sbuf[n] = total_of(o).astype(BF16)
            rs_copy(o, sbuf.at[n]).start()
        if l == 0:
            for name in ("gs", "us", "ds", "og"):
                loads[name].wait()
            cast(0, ("wd",))
        rcol[...] = ss_end().reshape(ttiles, ROWS, LANES)
        acc = total_of(0)

        first = start_of(z)
        for k in range(take):
            t = first + k
            i, j = lax.rem(t, ttiles), t // ttiles
            rinv = rcol[i]
            at_j = pl.ds(pl.multiple_of(j * LANES, LANES), LANES)
            gate = acc[k, 0] * rinv * gs[l : l + 1, at_j]
            up = acc[k, 1] * rinv * us[l : l + 1, at_j]
            hall[z, k] = (gate / (1.0 + jnp.exp(-gate)) * up).astype(BF16)

        forwards = set(DOWN.values())

        def ag_copy(o, owner):
            return pltpu.make_async_remote_copy(
                src_ref=hall.at[owner], dst_ref=hall.at[owner], send_sem=ag_s, recv_sem=ag_r.at[EDGE[o] if o in forwards else len(EDGE)],
                device_id={"ra": at(o - DOWN[o])}, device_id_type=MESH)

        held = {0}
        for c, o in DOWN.items():
            if o not in held:
                if l == 0 and len(held) == 1:
                    for ll in range(1, layers):
                        cast(ll, ("wg", "wu", "wd"))
                ag_copy(o, at(-o)).wait_recv()
                held.add(o)
            ag_copy(c, at(-o)).start()
        wait_for(hall.at[pl.ds(0, sum(o not in forwards for o in DOWN))], ag_r.at[len(EDGE)])
        place = []
        for t in range(tiles):
            owner = max(p for p in range(n_ra) if start_of(p) <= t)
            place.append((owner, t - start_of(owner)))
        hidden = jnp.concatenate(
            [jnp.concatenate([hall[p, k] for p, k in place[j * ttiles : (j + 1) * ttiles]], axis=0) for j in range(cols)],
            axis=1)
        terms = jnp.dot(hidden, wdb[l], preferred_element_type=F32)
        cbuf[l, me] = terms.astype(BF16)

        def cb_copy(k, slot):
            return pltpu.make_async_remote_copy(
                src_ref=cbuf.at[l, slot], dst_ref=cbuf.at[l, slot], send_sem=cb_s.at[l], recv_sem=cb_r.at[l],
                device_id={"cb": lax.rem(me + k, n_cb)}, device_id_type=MESH)

        for k in range(1, n_cb):
            cb_copy(k, me).start()
        wait_for(rbuf, rs_s)
        wait_for(ssr, ss_s)
        wait_for(hall.at[pl.ds(0, len(DOWN))], ag_s)
        wait_for(cbuf.at[l, pl.ds(0, n_cb - 1)], cb_r.at[l])
        branch = cbuf[l, 0].astype(F32)
        for k in range(1, n_cb):
            branch = branch + cbuf[l, k].astype(F32)
        wait_for(cbuf.at[l, pl.ds(0, n_cb - 1)], cb_s.at[l])
        x_ref[...] = (0.5 * xf + branch * ds[l : l + 1, :]).astype(BF16).astype(F32)

    xf = x_ref[...]
    fin[0:1] = jnp.sum((xf * xf).T, axis=0, keepdims=True)

    def fin_copy(d):
        k = d % n_ra
        return pltpu.make_async_remote_copy(
            src_ref=fin.at[pl.ds(0, 1)], dst_ref=fin.at[pl.ds(k, 1)], send_sem=fin_s, recv_sem=fin_r,
            device_id={"ra": at(d)}, device_id_type=MESH)

    far = [s * d for d in range(n_ra // 2, 0, -1) for s in (1, -1) if 2 * d < n_ra or s > 0]
    for d in far:
        fin_copy(d).start()
    scaled = xf * og[...]
    wait_for(fin.at[pl.ds(0, n_ra - 1)], fin_r)
    rinv = lax.rsqrt(jnp.sum(fin[...], axis=0, keepdims=True) / width + eps)
    o_ref[...] = (scaled * jnp.broadcast_to(rinv, (LANES, tok)).T).astype(BF16)
    wait_for(fin.at[pl.ds(0, n_ra - 1)], fin_s)


def solution(mesh):
    n_ra, n_cb = mesh.shape["ra"], mesh.shape["cb"]

    def local(stream, w_gate, w_up, w_down, gate_scale, up_scale, down_scale, pre_gain, out_gain):
        layers, d_own, ff = w_gate.shape
        tok = stream.shape[0]
        tiles = (ff // LANES) * (tok // ROWS)
        take = -(-tiles // n_ra)
        edges = len(EDGE)
        dma = pltpu.SemaphoreType.DMA
        scratch = [
            pltpu.VMEM(stream.shape, BF16),
            pltpu.VMEM(w_gate.shape, F32),
            pltpu.VMEM(w_up.shape, F32),
            pltpu.VMEM(w_down.shape, F32),
            pltpu.VMEM(gate_scale.shape, F32),
            pltpu.VMEM(up_scale.shape, F32),
            pltpu.VMEM(down_scale.shape, F32),
            pltpu.VMEM(pre_gain.shape, F32),
            pltpu.VMEM((1, d_own), F32),
            pltpu.VMEM(w_gate.shape, BF16),
            pltpu.VMEM(w_up.shape, BF16),
            pltpu.VMEM(w_down.shape, BF16),
            pltpu.VMEM(stream.shape, F32),
            pltpu.VMEM((tiles, 2, ROWS, LANES), BF16),
            pltpu.VMEM((edges, take, 2, ROWS, LANES), BF16),
            pltpu.VMEM((len(INNER), take, 2, ROWS, LANES), BF16),
            pltpu.VMEM((n_ra, take, ROWS, LANES), BF16),
            pltpu.VMEM((layers, n_cb, tok, d_own), BF16),
            pltpu.VMEM((6, 8, tok), F32),
            pltpu.VMEM((len(WINDOWS), 8, tok), F32),
            pltpu.VMEM((tok // ROWS, ROWS, LANES), F32),
            dma((6 + 3 * layers,)),
            dma, dma((len(NODE),)), dma, dma((edges + 1,)),
            dma((layers,)), dma((layers,)),
            dma, dma((len(WINDOWS),)),
            pltpu.VMEM((n_ra, tok), F32), dma, dma,
        ]
        kernel = functools.partial(body, n_ra, n_cb, layers, n_ra * d_own, 1e-6)
        return pl.pallas_call(
            lambda *refs: kernel(refs),
            out_shape=jax.ShapeDtypeStruct(stream.shape, BF16),
            in_specs=[pl.BlockSpec(memory_space=pl.ANY)] * 9,
            out_specs=pl.BlockSpec(memory_space=pltpu.VMEM),
            scratch_shapes=scratch,
            name="ffn_pair",
            compiler_params=pltpu.CompilerParams(collective_id=0, has_side_effects=True),
        )(stream, w_gate, w_up, w_down, gate_scale, up_scale, down_scale, pre_gain, out_gain.reshape(1, d_own))

    placed = (
        P("grp", "ra"),
        P(None, "ra", "cb"),
        P(None, "ra", "cb"),
        P(None, "cb", "ra"),
        P(None, "cb"),
        P(None, "cb"),
        P(None, "ra"),
        P(None, "ra"),
        P("ra"),
    )
    return jax.shard_map(local, mesh=mesh, in_specs=placed, out_specs=P("grp", "ra"), check_vma=False)
```

```python
import functools

import jax
import jax.numpy as jnp
from jax import lax
from jax.experimental import pallas as pl
from jax.experimental.pallas import tpu as pltpu
from jax.sharding import PartitionSpec as P

MESH = pl.DeviceIdType.MESH
F32, BF16 = jnp.float32, jnp.bfloat16
LANES, ROWS = 128, 16

UP = {-11: -9, -14: -13, 10: 11, -7: -8, 2: 1, 16: 13, 12: 13, -15: -12, 14: 13, 15: 13, -13: -12, -8: -9, -1: 0,
    -4: -5, 6: 7, 5: 4, -6: -5, -10: -9, 11: 9, 13: 8, -12: -9, 7: 8, 9: 8, 3: 1, -3: -2, -5: -2, 4: 1, -9: 0, 8: 0,
    1: 0, -2: 0}
DOWN = {9: 0, -4: 0, -9: 0, 7: 0, -11: -4, -7: -4, -2: -4, 2: 0, -3: -4, 3: 0, 6: 7, 1: 0, 8: 7, 12: 9, -12: -9, 10: 9,
    16: 9, -15: -9, -6: -7, 4: 6, 5: 6, -10: -9, -8: -7, -1: 0, 13: 9, 15: 12, 14: 12, 11: 10, -5: -4, -13: -12,
    -14: -12}
SUMMED = {}
for _o, _q in UP.items():
    SUMMED.setdefault(_q, []).append(_o)
EDGE = {o: k for k, o in enumerate(c for q in SUMMED for c in SUMMED[q])}
NODE = {q: k for k, q in enumerate(SUMMED)}
INNER = [o for o in UP if o in SUMMED]
WINDOWS = ((1, "own"), (-1, "own"), (3, "near"), (-3, "near"), (-6, "near"), (5, "pair"), (-9, "right"), (9, "left"))
REACH = {abs(o - q) for tree in (UP, DOWN) for o, q in tree.items()} | {abs(d) for d, _ in WINDOWS}
PEERS = sorted(s * d for d in REACH for s in (1, -1))


def body(n_ra, n_cb, layers, width, eps, refs):
    (x_hbm, wg_hbm, wu_hbm, wd_hbm, gs_hbm, us_hbm, ds_hbm, pg_hbm, og_hbm, o_ref,
     x_in, wg, wu, wd, gs, us, ds, pg, og, wgb, wub, wdb, x_ref, pbuf, rbuf, sbuf, hall, cbuf, ssb, ssr, rcol,
     in_sem, rs_s, rs_r, ag_s, ag_r, cb_s, cb_r, ss_s, ss_r, fin, fin_s, fin_r) = refs
    z, me = lax.axis_index("ra"), lax.axis_index("cb")
    ff = wg.shape[2]
    cols = ff // LANES
    tok = x_ref.shape[0]
    ttiles = tok // ROWS
    tiles = cols * ttiles
    take = rbuf.shape[1]

    def at(d):
        return lax.rem(z + (n_ra + d), n_ra)

    def start_of(owner):
        return owner * tiles // n_ra

    barrier = pltpu.get_barrier_semaphore()
    for d in PEERS:
        pl.semaphore_signal(barrier, inc=1, device_id={"ra": at(d)}, device_id_type=MESH)
    for k in range(1, n_cb):
        pl.semaphore_signal(barrier, inc=1, device_id={"cb": lax.rem(me + k, n_cb)}, device_id_type=MESH)

    loads = {}

    def load(name, src, dst):
        loads[name] = pltpu.make_async_copy(src, dst, in_sem.at[len(loads)])
        loads[name].start()

    load("x", x_hbm, x_in)
    load("pg", pg_hbm, pg)
    load(("wg", 0), wg_hbm.at[0], wg.at[0])
    load(("wu", 0), wu_hbm.at[0], wu.at[0])

    def load_rest():
        load("gs", gs_hbm, gs)
        load("us", us_hbm, us)
        load("ds", ds_hbm, ds)
        load("og", og_hbm, og)
        load(("wd", 0), wd_hbm.at[0], wd.at[0])
        for l in range(1, layers):
            load(("wg", l), wg_hbm.at[l], wg.at[l])
            load(("wu", l), wu_hbm.at[l], wu.at[l])
            load(("wd", l), wd_hbm.at[l], wd.at[l])

    def wait_for(ref, sem):
        pltpu.make_async_copy(ref, ref, sem).wait()

    def cast(l, which):
        for name, src, dst in (("wg", wg, wgb), ("wu", wu, wub), ("wd", wd, wdb)):
            if name in which:
                loads[(name, l)].wait()
                dst[l] = src[l].astype(BF16)

    def rs_copy(o, src):
        return pltpu.make_async_remote_copy(
            src_ref=src, dst_ref=rbuf.at[EDGE[o]], send_sem=rs_s, recv_sem=rs_r.at[NODE[UP[o]]],
            device_id={"ra": at(UP[o] - o)}, device_id_type=MESH)

    def ss_copy(k):
        kind = {"own": 0, "near": 1, "pair": 2, "right": 3, "left": 4}[WINDOWS[k][1]]
        return pltpu.make_async_remote_copy(
            src_ref=ssb.at[kind], dst_ref=ssr.at[k], send_sem=ss_s, recv_sem=ss_r.at[k],
            device_id={"ra": at(WINDOWS[k][0])}, device_id_type=MESH)

    def ss_own(xf):
        own = jnp.sum((xf * xf).T, axis=0, keepdims=True)
        ssb[0] = jnp.broadcast_to(own, ssb.shape[1:])

    def ss_start():
        for k in (0, 1):
            ss_copy(k).start()

    def ss_near():
        for k in (0, 1):
            ss_copy(k).wait_recv()
        ssb[1] = ssb[0] + ssr[0] + ssr[1]
        ssb[2] = ssb[0] + ssr[0]
        for k in (4, 5, 2, 3):
            ss_copy(k).start()

    def ss_mid():
        for k in (2, 3, 4, 5):
            ss_copy(k).wait_recv()
        nine = ssb[1] + ssr[2] + ssr[3]
        ssb[3] = nine + ssr[4]
        ssb[4] = nine + ssr[5]
        ssb[5] = nine
        for k in (6, 7):
            ss_copy(k).start()

    def ss_end():
        for k in (6, 7):
            ss_copy(k).wait_recv()
        total = ssb[5] + ssr[6] + ssr[7]
        rinv = lax.rsqrt(total[0:1] / width + eps)
        return jnp.broadcast_to(rinv, (LANES, tok)).T

    loads["x"].wait()
    x_ref[...] = x_in[...].astype(F32)

    for l in range(layers):
        xf = x_ref[...]
        ss_own(xf)
        if l > 0:
            ss_start()
        if l == 0:
            loads["pg"].wait()
            cast(0, ("wg", "wu"))
        scaled = (xf * pg[l : l + 1, :]).astype(BF16)
        for which, w in ((0, wgb), (1, wub)):
            part = jnp.dot(scaled, w[l], preferred_element_type=F32).astype(BF16)
            for j in range(cols):
                pbuf[j * ttiles : (j + 1) * ttiles, which] = part[:, j * LANES : (j + 1) * LANES].reshape(
                    ttiles, ROWS, LANES)
        if l == 0:
            pl.semaphore_wait(barrier, len(PEERS) + n_cb - 1)
            ss_start()

        def total_of(o):
            wait_for(rbuf.at[pl.ds(EDGE[SUMMED[o][0]], len(SUMMED[o]))], rs_r.at[NODE[o]])
            acc = pbuf[pl.ds(start_of(at(-o)), take)].astype(F32)
            for c in SUMMED[o]:
                acc = acc + rbuf[EDGE[c]].astype(F32)
            return acc

        for o in UP:
            if o not in SUMMED:
                rs_copy(o, pbuf.at[pl.ds(start_of(at(-o)), take)]).start()
                continue
            n = INNER.index(o)
            if n == 0:
                if l == 0:
                    load_rest()
                ss_near()
            if n == len(INNER) // 2:
                ss_mid()
            sbuf[n] = total_of(o).astype(BF16)
            rs_copy(o, sbuf.at[n]).start()
        if l == 0:
            for name in ("gs", "us", "ds", "og"):
                loads[name].wait()
            cast(0, ("wd",))
        rcol[...] = ss_end().reshape(ttiles, ROWS, LANES)
        acc = total_of(0)

        first = start_of(z)
        for k in range(take):
            t = first + k
            i, j = lax.rem(t, ttiles), t // ttiles
            rinv = rcol[i]
            at_j = pl.ds(pl.multiple_of(j * LANES, LANES), LANES)
            gate = acc[k, 0] * rinv * gs[l : l + 1, at_j]
            up = acc[k, 1] * rinv * us[l : l + 1, at_j]
            hall[z, k] = (gate / (1.0 + jnp.exp(-gate)) * up).astype(BF16)

        forwards = set(DOWN.values())

        def ag_copy(o, owner):
            return pltpu.make_async_remote_copy(
                src_ref=hall.at[owner], dst_ref=hall.at[owner], send_sem=ag_s, recv_sem=ag_r.at[EDGE[o] if o in forwards else len(EDGE)],
                device_id={"ra": at(o - DOWN[o])}, device_id_type=MESH)

        held = {0}
        for c, o in DOWN.items():
            if o not in held:
                if l == 0 and len(held) == 1:
                    for ll in range(1, layers):
                        cast(ll, ("wg", "wu", "wd"))
                ag_copy(o, at(-o)).wait_recv()
                held.add(o)
            ag_copy(c, at(-o)).start()
        wait_for(hall.at[pl.ds(0, sum(o not in forwards for o in DOWN))], ag_r.at[len(EDGE)])
        place = []
        for t in range(tiles):
            owner = max(p for p in range(n_ra) if start_of(p) <= t)
            place.append((owner, t - start_of(owner)))
        hidden = jnp.concatenate(
            [jnp.concatenate([hall[p, k] for p, k in place[j * ttiles : (j + 1) * ttiles]], axis=0) for j in range(cols)],
            axis=1)
        terms = jnp.dot(hidden, wdb[l], preferred_element_type=F32)
        cbuf[l, me] = terms.astype(BF16)

        def cb_copy(k, slot):
            return pltpu.make_async_remote_copy(
                src_ref=cbuf.at[l, slot], dst_ref=cbuf.at[l, slot], send_sem=cb_s.at[l], recv_sem=cb_r.at[l],
                device_id={"cb": lax.rem(me + k, n_cb)}, device_id_type=MESH)

        for k in sorted(range(1, n_cb), key=lambda k: -min(k, n_cb - k)):
            cb_copy(k, me).start()
        wait_for(rbuf, rs_s)
        wait_for(ssr, ss_s)
        wait_for(hall.at[pl.ds(0, len(DOWN))], ag_s)
        wait_for(cbuf.at[l, pl.ds(0, n_cb - 1)], cb_r.at[l])
        branch = cbuf[l, 0].astype(F32)
        for k in range(1, n_cb):
            branch = branch + cbuf[l, k].astype(F32)
        wait_for(cbuf.at[l, pl.ds(0, n_cb - 1)], cb_s.at[l])
        x_ref[...] = (0.5 * xf + branch * ds[l : l + 1, :]).astype(BF16).astype(F32)

    xf = x_ref[...]
    fin[0:1] = jnp.sum((xf * xf).T, axis=0, keepdims=True)

    def fin_copy(d):
        k = d % n_ra
        return pltpu.make_async_remote_copy(
            src_ref=fin.at[pl.ds(0, 1)], dst_ref=fin.at[pl.ds(k, 1)], send_sem=fin_s, recv_sem=fin_r,
            device_id={"ra": at(d)}, device_id_type=MESH)

    far = [s * d for d in range(n_ra // 2, 0, -1) for s in (1, -1) if 2 * d < n_ra or s > 0]
    for d in far:
        fin_copy(d).start()
    scaled = xf * og[...]
    wait_for(fin.at[pl.ds(0, n_ra - 1)], fin_r)
    rinv = lax.rsqrt(jnp.sum(fin[...], axis=0, keepdims=True) / width + eps)
    o_ref[...] = (scaled * jnp.broadcast_to(rinv, (LANES, tok)).T).astype(BF16)
    wait_for(fin.at[pl.ds(0, n_ra - 1)], fin_s)


def solution(mesh):
    n_ra, n_cb = mesh.shape["ra"], mesh.shape["cb"]

    def local(stream, w_gate, w_up, w_down, gate_scale, up_scale, down_scale, pre_gain, out_gain):
        layers, d_own, ff = w_gate.shape
        tok = stream.shape[0]
        tiles = (ff // LANES) * (tok // ROWS)
        take = -(-tiles // n_ra)
        edges = len(EDGE)
        dma = pltpu.SemaphoreType.DMA
        scratch = [
            pltpu.VMEM(stream.shape, BF16),
            pltpu.VMEM(w_gate.shape, F32),
            pltpu.VMEM(w_up.shape, F32),
            pltpu.VMEM(w_down.shape, F32),
            pltpu.VMEM(gate_scale.shape, F32),
            pltpu.VMEM(up_scale.shape, F32),
            pltpu.VMEM(down_scale.shape, F32),
            pltpu.VMEM(pre_gain.shape, F32),
            pltpu.VMEM((1, d_own), F32),
            pltpu.VMEM(w_gate.shape, BF16),
            pltpu.VMEM(w_up.shape, BF16),
            pltpu.VMEM(w_down.shape, BF16),
            pltpu.VMEM(stream.shape, F32),
            pltpu.VMEM((tiles, 2, ROWS, LANES), BF16),
            pltpu.VMEM((edges, take, 2, ROWS, LANES), BF16),
            pltpu.VMEM((len(INNER), take, 2, ROWS, LANES), BF16),
            pltpu.VMEM((n_ra, take, ROWS, LANES), BF16),
            pltpu.VMEM((layers, n_cb, tok, d_own), BF16),
            pltpu.VMEM((6, 8, tok), F32),
            pltpu.VMEM((len(WINDOWS), 8, tok), F32),
            pltpu.VMEM((tok // ROWS, ROWS, LANES), F32),
            dma((6 + 3 * layers,)),
            dma, dma((len(NODE),)), dma, dma((edges + 1,)),
            dma((layers,)), dma((layers,)),
            dma, dma((len(WINDOWS),)),
            pltpu.VMEM((n_ra, tok), F32), dma, dma,
        ]
        kernel = functools.partial(body, n_ra, n_cb, layers, n_ra * d_own, 1e-6)
        return pl.pallas_call(
            lambda *refs: kernel(refs),
            out_shape=jax.ShapeDtypeStruct(stream.shape, BF16),
            in_specs=[pl.BlockSpec(memory_space=pl.ANY)] * 9,
            out_specs=pl.BlockSpec(memory_space=pltpu.VMEM),
            scratch_shapes=scratch,
            name="ffn_pair",
            compiler_params=pltpu.CompilerParams(collective_id=0, has_side_effects=True),
        )(stream, w_gate, w_up, w_down, gate_scale, up_scale, down_scale, pre_gain, out_gain.reshape(1, d_own))

    placed = (
        P("grp", "ra"),
        P(None, "ra", "cb"),
        P(None, "ra", "cb"),
        P(None, "cb", "ra"),
        P(None, "cb"),
        P(None, "cb"),
        P(None, "ra"),
        P(None, "ra"),
        P("ra"),
    )
    return jax.shard_map(local, mesh=mesh, in_specs=placed, out_specs=P("grp", "ra"), check_vma=False)
```
